32 devices in a mesh: ep: 8 (over z, core), tp: 4 (over y, x).
Axes of the slice: x: 2, y: 2, z: 4, core: 2. Of those that a mesh axis runs over, the one named last changes fastest.
Arguments:
- reception_vectors: bfloat16 [1024, 2048], P('ep', 'tp'), may hold values from -6 to 6
- lookup_vectors: bfloat16 [1024, 2048], P('ep', 'tp'), may hold values from -0.75 to 0.75
- payload_vectors: bfloat16 [1024, 2048], P('ep', 'tp'), may hold values from -6 to 6
- fix_strength_signal: bfloat16 [1024, 2048], P('ep', 'tp'), may hold values from -5 to 5
- fade_signal_term: bfloat16 [1024, 2048], P('ep', 'tp'), may hold values from -8 to 8
- state_erasure: bfloat16 [1024, 2048], P('ep', 'tp'), may hold values from 0 to 1
- feature_speed_pairs: float32 [2, 2048], P(None, 'tp'), as said below
- subspace_scale_vector: float32 [2048], P('tp'), may hold values from 0.1 to 1.9
- subspace_merge_matrix: bfloat16 [2048, 4096], P(None, 'tp'), may hold values from -0.125 to 0.125
- specialist_entry_vectors: bfloat16 [512, 4096], P('ep'), may hold values from -6 to 6
- specialist_entry_scale: float32 [4096], replicated, may hold values from 0.1 to 1.9
- specialist_picks: int32 [512, 2], P('ep'), may hold values from 0 to 7, as said below
- dispatch_replica_share: float32 [512, 2], P('ep'), may hold values from 0.2 to 1
- specialist_valve_matrix: bfloat16 [8, 4096, 2048], P('ep', None, 'tp'), may hold values from -0.09375 to 0.09375
- specialist_raising_matrix: bfloat16 [8, 4096, 2048], P('ep', None, 'tp'), may hold values from -0.09375 to 0.09375
- specialist_lowering_matrix: bfloat16 [8, 2048, 4096], P('ep', None, 'tp'), may hold values from -0.125 to 0.125
Outputs:
- sequence_blend_result: bfloat16 [1024, 4096], P('ep', 'tp')
- expert_out: bfloat16 [512, 4096], P('ep', 'tp')
The draws below stay inside these ranges and needn't reach their ends.
Inputs may be any that keep to these rules, and one draw needn't show every extreme that they name: `specialist_picks`: the two experts of a row differ and lie in one group, experts g * 2 to g * 2 + 1 for some g. Among the rows of one device (aligned blocks of 64 rows) no expert is named more than 24 times, and some expert exactly 24 times. `feature_speed_pairs`: Finite.
All inputs are finite; a program needn't handle non-finite values.
Results may differ from the reference program's by a relative error of at most 0.0071.
Values may be sent and summed in bfloat16 or wider, within the bound.
A program may use at most 128 MiB of HBM per device.

```python
import math
import jax
import jax.numpy as jnp
from jax import lax

D = 4096
HEAD = 64
WIDTH = 2048
FF = 2048
GROUPS = 4
TOPK = 2
EXPERTS = 8
SPAN = 128
SEQ_A = 1024
TB = 64
TOK_B = 512
BUSIEST = 24
CAP = 24
N_EP = 8


def draw_feature_speed_pairs(key, part):
    head_count = WIDTH // HEAD
    first, second, third = jax.random.split(key, 3)
    slow_heads = jax.random.uniform(first, (head_count,), jnp.float32) < 0.5
    slow_decay = math.log(0.15 / SEQ_A)
    slow_chan = jnp.repeat(slow_heads, HEAD)
    decay_row = jnp.where(slow_chan, slow_decay, math.log(1.0 / 80.0))
    decay_row = decay_row + jax.random.uniform(second, (WIDTH,), jnp.float32, -0.35, 0.35)
    learn_row = jnp.where(slow_chan, math.log(0.25 * HEAD / SEQ_A), -1.0)
    learn_row = learn_row + jax.random.uniform(third, (WIDTH,), jnp.float32, -0.5, 0.5)
    return jnp.stack([decay_row, learn_row]).astype(jnp.float32)


def draw_fade_signal_term(key, part):
    first, second = jax.random.split(key)
    noise_part = jax.random.normal(first, (SEQ_A, WIDTH), jnp.float32)
    shift_by = jax.random.uniform(second, (N_EP,), jnp.float32, -0.7, 0.7)
    return (noise_part + jnp.repeat(shift_by, SPAN)[:, None]).astype(jnp.bfloat16)


def draw_state_erasure(key, part):
    head_count = WIDTH // HEAD
    first, second = jax.random.split(key)
    where_at = jax.random.randint(first, (head_count, 2), 0, SEQ_A)
    lost_share = jax.random.uniform(second, (head_count, 2), jnp.float32, 0.2, 0.4)
    strength = -jnp.log(1.0 - lost_share)
    hits = (jnp.arange(SEQ_A)[:, None, None] == where_at[None]).astype(jnp.float32) * strength[None]
    per_head = jnp.sum(hits, axis=2)
    return jnp.repeat(per_head, HEAD, axis=1).astype(jnp.bfloat16)


def permute_block(subkey):
    return jax.random.permutation(subkey, TB)


def draw_specialist_picks(key, part):
    blocks = TOK_B // TB
    per_group = EXPERTS // GROUPS
    remaining = TB - BUSIEST
    subkeys = jax.random.split(key, 7)
    top_group = jax.random.randint(subkeys[0], (blocks,), 0, GROUPS)
    group_iota = jnp.arange(GROUPS, dtype=jnp.int32)
    scores = jax.random.randint(subkeys[1], (blocks, GROUPS), 1, 1 << 20) * GROUPS + group_iota[None, :]
    scores = jnp.where(group_iota[None, :] == top_group[:, None], 0, scores)
    group_order = jnp.argsort(scores, axis=1).astype(jnp.int32)
    second_size = jax.random.randint(subkeys[2], (blocks,), max(0, remaining - 2 * BUSIEST), min(BUSIEST, remaining) + 1)
    third_size = jax.random.randint(subkeys[3], (blocks,), jnp.maximum(0, remaining - second_size - BUSIEST), jnp.minimum(BUSIEST, remaining - second_size) + 1)
    bounds = jnp.stack([jnp.zeros((blocks,), jnp.int32), jnp.full((blocks,), BUSIEST, jnp.int32), BUSIEST + second_size, BUSIEST + second_size + third_size], axis=1).astype(jnp.int32)
    position = jnp.arange(TB, dtype=jnp.int32)
    which = (position[None, :] >= bounds[:, 1:2]).astype(jnp.int32) + (position[None, :] >= bounds[:, 2:3]).astype(jnp.int32) + (position[None, :] >= bounds[:, 3:4]).astype(jnp.int32)
    group_id = jnp.take_along_axis(group_order, which, axis=1)
    start_of = jnp.take_along_axis(bounds, which, axis=1)
    rank_in = position[None, :] - start_of
    rotate = jax.random.randint(subkeys[4], (blocks, GROUPS), 0, per_group)
    step_off = jax.random.randint(subkeys[5], (blocks, GROUPS), 1, per_group)
    rot_row = jnp.take_along_axis(rotate, group_id, axis=1)
    off_row = jnp.take_along_axis(step_off, group_id, axis=1)
    first_e = group_id * per_group + (rank_in + rot_row) % per_group
    second_e = group_id * per_group + (rank_in + rot_row + off_row) % per_group
    paired = jnp.stack([first_e, second_e], axis=2)
    shuffle = jax.vmap(permute_block)(jax.random.split(subkeys[6], blocks))
    paired = jnp.take_along_axis(paired, shuffle[:, :, None], axis=1)
    return paired.reshape(TOK_B, 2).astype(jnp.int32)


def level_of(own_key, dims, pieces, low, high):
    level, own = 1.0, jax.random.fold_in(own_key, 6)
    for dim, blocks in pieces:
        draws = jnp.exp(jax.random.uniform(jax.random.fold_in(own, dim), (blocks,), jnp.float32, low / len(pieces), high / len(pieces)))
        level = level * jnp.repeat(draws, dims[dim] // blocks).reshape([-1 if axis == dim else 1 for axis in range(len(dims))])
    return level


def scatter_about(rng, dims, width, reach, shards=(), kind=jnp.bfloat16):
    loudness = level_of(rng, dims, shards, -0.22, 0.18) if shards else 1.0
    values = jax.random.normal(rng, dims, jnp.float32) * width * loudness
    return jnp.minimum(jnp.maximum(values, -reach), reach).astype(kind)


def setup_inputs(seed: int = 0) -> dict:
    seeds = jax.random.split(jax.random.key(seed), 17)
    reception_vectors = scatter_about(seeds[0], (SEQ_A, WIDTH), 1.0, 6.0, ((0, 8), (1, 4)))
    lookup_vectors = scatter_about(seeds[1], (SEQ_A, WIDTH), 0.125, 0.75, ((0, 8), (1, 4)))
    payload_vectors = scatter_about(seeds[2], (SEQ_A, WIDTH), 1.0, 6.0, ((0, 8), (1, 4)))
    fix_strength_signal = scatter_about(seeds[3], (SEQ_A, WIDTH), 1.0, 5.0, ((0, 8), (1, 4)))
    fade_signal_term = draw_fade_signal_term(jax.random.fold_in(seeds[16], 71), 0)
    state_erasure = draw_state_erasure(jax.random.fold_in(seeds[16], 71), 0)
    feature_speed_pairs = draw_feature_speed_pairs(jax.random.fold_in(seeds[16], 71), 0)
    subspace_scale_vector = jnp.clip(1.0 + 0.18 * jax.random.normal(seeds[7], (WIDTH,), jnp.float32), 0.1, 1.9)
    subspace_merge_matrix = scatter_about(seeds[8], (WIDTH, D), WIDTH ** -0.5, 0.125, ((1, 4),))
    specialist_entry_vectors = scatter_about(seeds[9], (TOK_B, D), 1.0, 6.0, ((0, 8),))
    specialist_entry_scale = jnp.clip(1.0 + 0.18 * jax.random.normal(seeds[10], (D,), jnp.float32), 0.1, 1.9)
    specialist_picks = draw_specialist_picks(jax.random.fold_in(seeds[16], 71), 0)
    dispatch_replica_share = jnp.clip(0.2 + 0.8 * jax.random.uniform(seeds[12], (TOK_B, TOPK), jnp.float32) ** level_of(seeds[12], (TOK_B, TOPK), ((0, 8),), -0.2, 0.2), 0.2, 1.0)
    specialist_valve_matrix = scatter_about(seeds[13], (EXPERTS, D, FF), D ** -0.5, 0.09375, ((0, 8), (2, 4)))
    specialist_raising_matrix = scatter_about(seeds[14], (EXPERTS, D, FF), D ** -0.5, 0.09375, ((0, 8), (2, 4)))
    specialist_lowering_matrix = scatter_about(seeds[15], (EXPERTS, FF, D), FF ** -0.5, 0.125, ((0, 8), (2, 4)))
    return dict(reception_vectors=reception_vectors, lookup_vectors=lookup_vectors, payload_vectors=payload_vectors, fix_strength_signal=fix_strength_signal, fade_signal_term=fade_signal_term, state_erasure=state_erasure, feature_speed_pairs=feature_speed_pairs, subspace_scale_vector=subspace_scale_vector, subspace_merge_matrix=subspace_merge_matrix, specialist_entry_vectors=specialist_entry_vectors, specialist_entry_scale=specialist_entry_scale, specialist_picks=specialist_picks, dispatch_replica_share=dispatch_replica_share, specialist_valve_matrix=specialist_valve_matrix, specialist_raising_matrix=specialist_raising_matrix, specialist_lowering_matrix=specialist_lowering_matrix)


highest = lax.Precision.HIGHEST

def blend_sequence(reception_vectors, lookup_vectors, payload_vectors, fix_strength_signal, fade_signal_term, state_erasure, feature_speed_pairs, subspace_scale_vector, subspace_merge_matrix):
    seq_len, channels = reception_vectors.shape
    head_count = channels // HEAD
    fade_speed_exponent = jnp.exp(-jnp.exp(feature_speed_pairs[0] + fade_signal_term.astype(jnp.float32)) - state_erasure.astype(jnp.float32))
    learn_rate = jax.nn.sigmoid(fix_strength_signal.astype(jnp.float32) + feature_speed_pairs[1])

    def split_heads(array):
        return array.astype(jnp.float32).reshape(seq_len, head_count, HEAD)
    key_heads = split_heads(lookup_vectors)
    key_unit = key_heads * lax.rsqrt(lax.optimization_barrier(jnp.sum(key_heads * key_heads, axis=-1, keepdims=True)) + 1e-06)

    def advance(state_mat, inputs):
        step_recept, step_decay, step_key, step_value, step_unit, step_learn = inputs
        state_hit = jnp.einsum('hvk,hk->hv', state_mat, step_unit, precision=highest)
        state_mat = state_mat * step_decay[:, None, :] - state_hit[:, :, None] * (step_unit * step_learn)[:, None, :] + step_value[:, :, None] * step_key[:, None, :]
        return (state_mat, jnp.einsum('hvk,hk->hv', state_mat, step_recept, precision=highest))
    initial = jnp.zeros((head_count, HEAD, HEAD), jnp.float32)
    final_state, outputs = lax.scan(advance, initial, (split_heads(reception_vectors), fade_speed_exponent.reshape(seq_len, head_count, HEAD), key_heads, split_heads(payload_vectors), key_unit, learn_rate.reshape(seq_len, head_count, HEAD)))
    head_mean = lax.optimization_barrier(jnp.mean(outputs, axis=-1, keepdims=True))
    centred = outputs - head_mean
    head_var = lax.optimization_barrier(jnp.mean(centred * centred, axis=-1, keepdims=True))
    scaled = centred * lax.rsqrt(head_var + 0.00064) * subspace_scale_vector.reshape(head_count, HEAD)
    mixed_rows = scaled.reshape(seq_len, channels).astype(jnp.bfloat16)
    return jnp.dot(mixed_rows, subspace_merge_matrix, preferred_element_type=jnp.float32).astype(jnp.bfloat16)

def expert_layer(specialist_entry_vectors, specialist_entry_scale, specialist_picks, dispatch_replica_share, specialist_valve_matrix, specialist_raising_matrix, specialist_lowering_matrix):
    widened = specialist_entry_vectors.astype(jnp.float32)
    normed = (widened * lax.rsqrt(lax.optimization_barrier(jnp.mean(widened * widened, axis=-1, keepdims=True)) + 1e-06) * specialist_entry_scale).astype(jnp.bfloat16)
    flat_ids = specialist_picks.reshape(-1).astype(jnp.int32)
    flat_weight = dispatch_replica_share.reshape(-1)
    token_of = (jnp.arange(flat_ids.shape[0], dtype=jnp.int32) // TOPK).astype(jnp.int32)
    max_rows = N_EP * CAP

    def run_expert(running, expert):
        order_idx = jnp.argsort((flat_ids != expert).astype(jnp.int32), stable=True)[:max_rows]
        chosen = token_of[order_idx]
        live_weight = jnp.where(flat_ids[order_idx] == expert, flat_weight[order_idx], 0.0)
        rows_in = normed[chosen]
        gate_part = jnp.dot(rows_in, specialist_valve_matrix[expert], preferred_element_type=jnp.float32)
        up_part = jnp.dot(rows_in, specialist_raising_matrix[expert], preferred_element_type=jnp.float32)
        hidden = (jax.nn.silu(gate_part) * up_part).astype(jnp.bfloat16)
        result = jnp.dot(hidden, specialist_lowering_matrix[expert], preferred_element_type=jnp.float32).astype(jnp.bfloat16)
        running = running.at[chosen].add(result.astype(jnp.float32) * live_weight[:, None])
        return (running, None)
    running, unused = lax.scan(run_expert, jnp.zeros(specialist_entry_vectors.shape, jnp.float32), jnp.arange(EXPERTS, dtype=jnp.int32))
    return running.astype(jnp.bfloat16)

def reference(reception_vectors, lookup_vectors, payload_vectors, fix_strength_signal, fade_signal_term, state_erasure, feature_speed_pairs, subspace_scale_vector, subspace_merge_matrix, specialist_entry_vectors, specialist_entry_scale, specialist_picks, dispatch_replica_share, specialist_valve_matrix, specialist_raising_matrix, specialist_lowering_matrix):
    sequence_blend_result = blend_sequence(reception_vectors, lookup_vectors, payload_vectors, fix_strength_signal, fade_signal_term, state_erasure, feature_speed_pairs, subspace_scale_vector, subspace_merge_matrix)
    expert_out = expert_layer(specialist_entry_vectors, specialist_entry_scale, specialist_picks, dispatch_replica_share, specialist_valve_matrix, specialist_raising_matrix, specialist_lowering_matrix)
    return (sequence_blend_result, expert_out)
```

```python
import jax
import jax.numpy as jnp
from jax import lax
from jax.experimental import pallas as pl
from jax.experimental.pallas import tpu as pltpu
from jax.sharding import PartitionSpec as P

HEAD = 64
GROUPS = 4


highest = lax.Precision.HIGHEST
BLOCK = 256


def split_pair(x):
    high = x.astype(jnp.bfloat16)
    return high, (x - high.astype(jnp.float32)).astype(jnp.bfloat16)


def dot_split(x, y, dims):
    x_high, x_low = split_pair(x)
    y_high, y_low = split_pair(y)

    def one(p, q):
        return lax.dot_general(p, q, (dims, ((), ())), preferred_element_type=jnp.float32)

    return one(x_high, y_high) + (one(x_high, y_low) + one(x_low, y_high))


ROWS = ((1,), (0,))
LAST = ((1,), (1,))
FIRST = ((0,), (0,))


def local_kernel(r_ref, k_ref, v_ref, fix_ref, fade_ref, loss_ref, speed_ref, own_ref, pair_ref):
    span, width = r_ref.shape
    heads = width // HEAD
    levels = span.bit_length() - 1
    decay = jnp.exp(
        -jnp.exp(speed_ref[0:1, :] + fade_ref[...].astype(jnp.float32))
        - loss_ref[...].astype(jnp.float32)
    )
    learn = jax.nn.sigmoid(fix_ref[...].astype(jnp.float32) + speed_ref[1:2, :])
    recept = r_ref[...].astype(jnp.float32)
    key = k_ref[...].astype(jnp.float32)
    squares = key * key
    lane_head = lax.broadcasted_iota(jnp.int32, (span, width), 1) // HEAD
    inverse = jnp.zeros((span, width), jnp.float32)
    for h in range(heads):
        mine = lane_head == h
        total = jnp.sum(jnp.where(mine, squares, 0.0), axis=1, keepdims=True)
        inverse = jnp.where(mine, lax.rsqrt(total + 1e-06), inverse)
    unit = key * inverse
    removal = unit * learn
    place = lax.broadcasted_iota(jnp.int32, (span, width), 0)
    row = lax.broadcasted_iota(jnp.int32, (2 * span, 2 * span), 0) % span
    col = lax.broadcasted_iota(jnp.int32, (2 * span, 2 * span), 1) % span
    small_row = lax.broadcasted_iota(jnp.int32, (span, span), 0)
    small_col = lax.broadcasted_iota(jnp.int32, (span, span), 1)
    eye = jnp.where(small_row == small_col, 1.0, 0.0)
    prefix, before, suffix, total = decay, jnp.ones_like(decay), jnp.ones_like(decay), decay
    scores = [jnp.zeros((2 * span, 2 * span), jnp.float32) for _ in range(heads)]
    solve = [eye for _ in range(heads)]
    for level in range(levels):
        size = 1 << level
        x_unit, x_recept = unit * before, recept * prefix
        y_key, y_removal = key * suffix, removal * suffix
        mask = (
            ((row >> (level + 1)) == (col >> (level + 1)))
            & (((row >> level) & 1) == 1)
            & (((col >> level) & 1) == 0)
        )
        parts = []
        for h in range(heads):
            cut = slice(h * HEAD, (h + 1) * HEAD)
            x = jnp.concatenate([x_unit[:, cut], x_recept[:, cut]], axis=0)
            y = jnp.concatenate([y_key[:, cut], y_removal[:, cut]], axis=0)
            part = jnp.where(mask, dot_split(x, y, LAST), 0.0)
            scores[h] = scores[h] + part
            parts.append(part[:span, span:])
        if level == 0:
            solve = [eye - part for part in parts]
        else:
            half = [dot_split(m, part, ROWS) for m, part in zip(solve, parts)]
            solve = [m - dot_split(q, m, ROWS) for m, q in zip(solve, half)]
        later = ((place >> level) & 1) == 1
        sibling = jnp.where(
            later, pltpu.roll(total, size, 0), pltpu.roll(total, span - size, 0)
        )
        prefix = jnp.where(later, prefix * sibling, prefix)
        before = jnp.where(later, before * sibling, before)
        suffix = jnp.where(later, suffix, suffix * sibling)
        total = total * sibling
    x_unit, x_recept = unit * before, recept * prefix
    y_key, y_removal = key * suffix, removal * suffix
    value = v_ref[...].astype(jnp.float32)
    same = recept * key
    taken = recept * removal
    head_eye = jnp.where(
        lax.broadcasted_iota(jnp.int32, (HEAD, HEAD), 0)
        == lax.broadcasted_iota(jnp.int32, (HEAD, HEAD), 1),
        1.0,
        0.0,
    )
    for h in range(heads):
        cut = slice(h * HEAD, (h + 1) * HEAD)
        both = scores[h]
        value_h = value[:, cut]
        same_h = jnp.sum(same[:, cut], axis=1, keepdims=True)
        taken_h = jnp.sum(taken[:, cut], axis=1, keepdims=True)
        from_value = dot_split(both[:, :span], value_h, ROWS)
        right = jnp.concatenate([from_value[:span], x_unit[:, cut]], axis=1)
        hit = dot_split(solve[h], right, ROWS)
        left = jnp.concatenate([from_value[span:] + same_h * value_h, x_recept[:, cut]], axis=1)
        left = left - dot_split(both[span:, span:], hit, ROWS) - taken_h * hit
        own_ref[:, 2 * h * HEAD : 2 * (h + 1) * HEAD] = left
        change = jnp.concatenate(
            [dot_split(value_h, y_key[:, cut], FIRST), head_eye * total[0:1, cut]], axis=0
        )
        pair_ref[:, cut] = change - dot_split(hit, y_removal[:, cut], FIRST)


def local_part(arrays, speeds):
    span, channels = arrays[0].shape
    width = min(channels, BLOCK)
    spec = pl.BlockSpec((span, width), lambda i: (0, i))
    return pl.pallas_call(
        local_kernel,
        grid=(channels // width,),
        in_specs=[spec] * 6 + [pl.BlockSpec((2, width), lambda i: (0, i))],
        out_specs=[
            pl.BlockSpec((span, 2 * width), lambda i: (0, i)),
            pl.BlockSpec((2 * HEAD, width), lambda i: (0, i)),
        ],
        out_shape=[
            jax.ShapeDtypeStruct((span, 2 * channels), jnp.float32),
            jax.ShapeDtypeStruct((2 * HEAD, channels), jnp.float32),
        ],
        cost_estimate=pl.CostEstimate(
            flops=channels * span * span * 40, bytes_accessed=span * channels * 26, transcendentals=0
        ),
        name="local_part",
    )(*arrays, speeds)


def finish_kernel(own_ref, pairs_ref, scale_ref, out_ref):
    span, channels = out_ref.shape
    heads = channels // HEAD
    place = lax.axis_index("ep")

    def one(step, states):
        after = []
        for h, state in enumerate(states):
            cut = slice(h * HEAD, (h + 1) * HEAD)
            later = pairs_ref[step, HEAD:, cut]
            after.append(dot_split(state, later, ROWS) + pairs_ref[step, :HEAD, cut])
        return tuple(after)

    zero = jnp.zeros((HEAD, HEAD), jnp.float32)
    states = lax.fori_loop(0, place, one, tuple(zero for _ in range(heads)))
    for h, state in enumerate(states):
        cut = slice(h * HEAD, (h + 1) * HEAD)
        own = own_ref[:, 2 * h * HEAD : (2 * h + 1) * HEAD]
        carried = own_ref[:, (2 * h + 1) * HEAD : 2 * (h + 1) * HEAD]
        out = own + dot_split(carried, state, LAST)
        centred = out - jnp.mean(out, axis=1, keepdims=True)
        var = jnp.mean(centred * centred, axis=1, keepdims=True)
        out_ref[:, cut] = (centred * lax.rsqrt(var + 0.00064) * scale_ref[0:1, cut]).astype(
            jnp.bfloat16
        )


def finish_part(own, pairs, scale):
    span, channels = own.shape[0], own.shape[1] // 2
    return pl.pallas_call(
        finish_kernel,
        out_shape=jax.ShapeDtypeStruct((span, channels), jnp.bfloat16),
        name="finish_part",
    )(own, pairs, scale)


def blend_sequence(
    reception_vectors,
    lookup_vectors,
    payload_vectors,
    fix_strength_signal,
    fade_signal_term,
    state_erasure,
    feature_speed_pairs,
    subspace_scale_vector,
    subspace_merge_matrix,
):
    own, pair = local_part(
        (
            reception_vectors,
            lookup_vectors,
            payload_vectors,
            fix_strength_signal,
            fade_signal_term,
            state_erasure,
        ),
        feature_speed_pairs,
    )
    pairs = lax.all_gather(pair, "ep")
    mixed_rows = finish_part(own, pairs, subspace_scale_vector.reshape(1, -1))
    return jnp.dot(
        lax.all_gather(mixed_rows, "tp", axis=1, tiled=True),
        subspace_merge_matrix,
        preferred_element_type=jnp.float32,
    ).astype(jnp.bfloat16)


def expert_layer(
    specialist_entry_vectors,
    specialist_entry_scale,
    specialist_picks,
    dispatch_replica_share,
    specialist_valve_matrix,
    specialist_raising_matrix,
    specialist_lowering_matrix,
):
    rows_here, model_width = specialist_entry_vectors.shape
    pairs = specialist_picks.shape[1]
    expert_count = lax.axis_size("ep") * specialist_valve_matrix.shape[0]
    per_group = expert_count // GROUPS
    busiest = per_group * max(1, 3 * rows_here // (8 * per_group))
    capacity = 2 * busiest // per_group
    widened = specialist_entry_vectors.astype(jnp.float32)
    normed = (
        widened
        * lax.rsqrt(jnp.mean(widened * widened, axis=-1, keepdims=True) + 1e-06)
        * specialist_entry_scale
    ).astype(jnp.bfloat16)
    flat_ids = specialist_picks.reshape(-1)
    onehot = (flat_ids[:, None] == jnp.arange(expert_count, dtype=jnp.int32)[None, :]).astype(
        jnp.int32
    )
    slot_rank = jnp.sum((jnp.cumsum(onehot, axis=0) - onehot) * onehot, axis=1)
    slot_index = flat_ids * capacity + slot_rank
    selected = jnp.arange(expert_count * capacity, dtype=jnp.int32)[:, None] == slot_index[None, :]
    selected = selected.reshape(expert_count * capacity, rows_here, pairs)
    placement_mat = jnp.any(selected, axis=-1).astype(jnp.bfloat16)
    combine_w = jnp.sum(selected.astype(jnp.float32) * dispatch_replica_share[None], axis=-1)
    send_rows = jnp.dot(placement_mat, normed, preferred_element_type=jnp.float32).astype(
        jnp.bfloat16
    )
    send_rows = send_rows.reshape(expert_count, capacity, model_width)
    arrived = lax.all_to_all(send_rows, "ep", split_axis=0, concat_axis=0, tiled=True)
    sources, item_count, feature_count = arrived.shape
    flat_rows = arrived.reshape(sources * item_count, feature_count)
    gate_part = jnp.dot(flat_rows, specialist_valve_matrix[0], preferred_element_type=jnp.float32)
    up_part = jnp.dot(flat_rows, specialist_raising_matrix[0], preferred_element_type=jnp.float32)
    hidden = (jax.nn.silu(gate_part) * up_part).astype(jnp.bfloat16)
    weight_rows = specialist_lowering_matrix[0]
    result = jnp.dot(
        lax.all_gather(hidden, "tp", axis=1, tiled=True),
        weight_rows,
        preferred_element_type=jnp.float32,
    ).astype(jnp.bfloat16)
    result = result.reshape(sources, item_count, specialist_lowering_matrix.shape[2])
    returned = lax.all_to_all(result, "ep", split_axis=0, concat_axis=0, tiled=True)
    flat_back = returned.reshape(expert_count * capacity, returned.shape[2]).astype(jnp.float32)
    combined = jnp.einsum("st,sd->td", combine_w, flat_back, precision=highest)
    return combined.astype(jnp.bfloat16)


def body(
    reception_vectors,
    lookup_vectors,
    payload_vectors,
    fix_strength_signal,
    fade_signal_term,
    state_erasure,
    feature_speed_pairs,
    subspace_scale_vector,
    subspace_merge_matrix,
    specialist_entry_vectors,
    specialist_entry_scale,
    specialist_picks,
    dispatch_replica_share,
    specialist_valve_matrix,
    specialist_raising_matrix,
    specialist_lowering_matrix,
):
    sequence_blend_result = blend_sequence(
        reception_vectors,
        lookup_vectors,
        payload_vectors,
        fix_strength_signal,
        fade_signal_term,
        state_erasure,
        feature_speed_pairs,
        subspace_scale_vector,
        subspace_merge_matrix,
    )
    expert_out = expert_layer(
        specialist_entry_vectors,
        specialist_entry_scale,
        specialist_picks,
        dispatch_replica_share,
        specialist_valve_matrix,
        specialist_raising_matrix,
        specialist_lowering_matrix,
    )
    return (sequence_blend_result, expert_out)


def solution(mesh):
    placed = (
        P("ep", "tp"),
        P("ep", "tp"),
        P("ep", "tp"),
        P("ep", "tp"),
        P("ep", "tp"),
        P("ep", "tp"),
        P(None, "tp"),
        P("tp"),
        P(None, "tp"),
        P("ep", None),
        P(),
        P("ep", None),
        P("ep", None),
        P("ep", None, "tp"),
        P("ep", None, "tp"),
        P("ep", None, "tp"),
    )
    return jax.shard_map(
        body, mesh=mesh, in_specs=placed, out_specs=(P("ep", "tp"), P("ep", "tp")), check_vma=False
    )
```

```python
import jax
import jax.numpy as jnp
from jax import lax
from jax.experimental import pallas as pl
from jax.experimental.pallas import tpu as pltpu
from jax.sharding import PartitionSpec as P

HEAD = 64
GROUPS = 4


highest = lax.Precision.HIGHEST
BLOCK = 256


def split_pair(x):
    high = x.astype(jnp.bfloat16)
    return high, (x - high.astype(jnp.float32)).astype(jnp.bfloat16)


def dot_split(x, y, dims):
    x_high, x_low = split_pair(x)
    y_high, y_low = split_pair(y)

    def one(p, q):
        return lax.dot_general(p, q, (dims, ((), ())), preferred_element_type=jnp.float32)

    return one(x_high, y_high) + (one(x_high, y_low) + one(x_low, y_high))


ROWS = ((1,), (0,))
LAST = ((1,), (1,))
FIRST = ((0,), (0,))


def local_kernel(r_ref, k_ref, v_ref, fix_ref, fade_ref, loss_ref, speed_ref, own_ref, pair_ref):
    span, width = r_ref.shape
    heads = width // HEAD
    levels = span.bit_length() - 1
    decay = jnp.exp(
        -jnp.exp(speed_ref[0:1, :] + fade_ref[...].astype(jnp.float32))
        - loss_ref[...].astype(jnp.float32)
    )
    learn = jax.nn.sigmoid(fix_ref[...].astype(jnp.float32) + speed_ref[1:2, :])
    recept = r_ref[...].astype(jnp.float32)
    key = k_ref[...].astype(jnp.float32)
    squares = key * key
    lane_head = lax.broadcasted_iota(jnp.int32, (span, width), 1) // HEAD
    inverse = jnp.zeros((span, width), jnp.float32)
    for h in range(heads):
        mine = lane_head == h
        total = jnp.sum(jnp.where(mine, squares, 0.0), axis=1, keepdims=True)
        inverse = jnp.where(mine, lax.rsqrt(total + 1e-06), inverse)
    unit = key * inverse
    removal = unit * learn
    place = lax.broadcasted_iota(jnp.int32, (span, width), 0)
    row = lax.broadcasted_iota(jnp.int32, (2 * span, 2 * span), 0) % span
    col = lax.broadcasted_iota(jnp.int32, (2 * span, 2 * span), 1) % span
    small_row = lax.broadcasted_iota(jnp.int32, (span, span), 0)
    small_col = lax.broadcasted_iota(jnp.int32, (span, span), 1)
    eye = jnp.where(small_row == small_col, 1.0, 0.0)
    prefix, before, suffix, total = decay, jnp.ones_like(decay), jnp.ones_like(decay), decay
    scores = [jnp.zeros((2 * span, 2 * span), jnp.float32) for _ in range(heads)]
    solve = [eye for _ in range(heads)]
    for level in range(levels):
        size = 1 << level
        x_unit, x_recept = unit * before, recept * prefix
        y_key, y_removal = key * suffix, removal * suffix
        mask = (
            ((row >> (level + 1)) == (col >> (level + 1)))
            & (((row >> level) & 1) == 1)
            & (((col >> level) & 1) == 0)
        )
        parts = []
        for h in range(heads):
            cut = slice(h * HEAD, (h + 1) * HEAD)
            x = jnp.concatenate([x_unit[:, cut], x_recept[:, cut]], axis=0)
            y = jnp.concatenate([y_key[:, cut], y_removal[:, cut]], axis=0)
            part = jnp.where(mask, dot_split(x, y, LAST), 0.0)
            scores[h] = scores[h] + part
            parts.append(part[:span, span:])
        if level == 0:
            solve = [eye - part for part in parts]
        else:
            half = [dot_split(m, part, ROWS) for m, part in zip(solve, parts)]
            solve = [m - dot_split(q, m, ROWS) for m, q in zip(solve, half)]
        later = ((place >> level) & 1) == 1
        sibling = jnp.where(
            later, pltpu.roll(total, size, 0), pltpu.roll(total, span - size, 0)
        )
        prefix = jnp.where(later, prefix * sibling, prefix)
        before = jnp.where(later, before * sibling, before)
        suffix = jnp.where(later, suffix, suffix * sibling)
        total = total * sibling
    x_unit, x_recept = unit * before, recept * prefix
    y_key, y_removal = key * suffix, removal * suffix
    value = v_ref[...].astype(jnp.float32)
    same = recept * key
    taken = recept * removal
    head_eye = jnp.where(
        lax.broadcasted_iota(jnp.int32, (HEAD, HEAD), 0)
        == lax.broadcasted_iota(jnp.int32, (HEAD, HEAD), 1),
        1.0,
        0.0,
    )
    for h in range(heads):
        cut = slice(h * HEAD, (h + 1) * HEAD)
        both = scores[h]
        value_h = value[:, cut]
        same_h = jnp.sum(same[:, cut], axis=1, keepdims=True)
        taken_h = jnp.sum(taken[:, cut], axis=1, keepdims=True)
        from_value = dot_split(both[:, :span], value_h, ROWS)
        right = jnp.concatenate([from_value[:span], x_unit[:, cut]], axis=1)
        hit = dot_split(solve[h], right, ROWS)
        left = jnp.concatenate([from_value[span:] + same_h * value_h, x_recept[:, cut]], axis=1)
        left = left - dot_split(both[span:, span:], hit, ROWS) - taken_h * hit
        own_ref[:, 2 * h * HEAD : 2 * (h + 1) * HEAD] = left
        change = jnp.concatenate(
            [dot_split(value_h, y_key[:, cut], FIRST), head_eye * total[0:1, cut]], axis=0
        )
        change = change - dot_split(hit, y_removal[:, cut], FIRST)
        pair_ref[:, cut] = change.astype(jnp.bfloat16)


def local_part(arrays, speeds):
    span, channels = arrays[0].shape
    width = min(channels, BLOCK)
    spec = pl.BlockSpec((span, width), lambda i: (0, i))
    return pl.pallas_call(
        local_kernel,
        grid=(channels // width,),
        in_specs=[spec] * 6 + [pl.BlockSpec((2, width), lambda i: (0, i))],
        out_specs=[
            pl.BlockSpec((span, 2 * width), lambda i: (0, i)),
            pl.BlockSpec((2 * HEAD, width), lambda i: (0, i)),
        ],
        out_shape=[
            jax.ShapeDtypeStruct((span, 2 * channels), jnp.float32),
            jax.ShapeDtypeStruct((2 * HEAD, channels), jnp.bfloat16),
        ],
        cost_estimate=pl.CostEstimate(
            flops=channels * span * span * 40, bytes_accessed=span * channels * 26, transcendentals=0
        ),
        name="local_part",
    )(*arrays, speeds)


def finish_kernel(own_ref, pairs_ref, scale_ref, out_ref):
    span, channels = out_ref.shape
    heads = channels // HEAD
    place = lax.axis_index("ep")

    def one(step, states):
        after = []
        for h, state in enumerate(states):
            cut = slice(h * HEAD, (h + 1) * HEAD)
            later = pairs_ref[step, HEAD:, cut]
            high, low = split_pair(state)
            both = jnp.concatenate([high, low], axis=0)
            moved = jnp.dot(both, later, preferred_element_type=jnp.float32)
            earned = pairs_ref[step, :HEAD, cut].astype(jnp.float32)
            after.append(moved[:HEAD] + moved[HEAD:] + earned)
        return tuple(after)

    zero = jnp.zeros((HEAD, HEAD), jnp.float32)
    states = lax.fori_loop(0, place, one, tuple(zero for _ in range(heads)))
    for h, state in enumerate(states):
        cut = slice(h * HEAD, (h + 1) * HEAD)
        own = own_ref[:, 2 * h * HEAD : (2 * h + 1) * HEAD]
        carried = own_ref[:, (2 * h + 1) * HEAD : 2 * (h + 1) * HEAD]
        out = own + dot_split(carried, state, LAST)
        centred = out - jnp.mean(out, axis=1, keepdims=True)
        var = jnp.mean(centred * centred, axis=1, keepdims=True)
        out_ref[:, cut] = (centred * lax.rsqrt(var + 0.00064) * scale_ref[0:1, cut]).astype(
            jnp.bfloat16
        )


def finish_part(own, pairs, scale):
    span, channels = own.shape[0], own.shape[1] // 2
    return pl.pallas_call(
        finish_kernel,
        out_shape=jax.ShapeDtypeStruct((span, channels), jnp.bfloat16),
        cost_estimate=pl.CostEstimate(
            flops=pairs.size * HEAD * 8, bytes_accessed=pairs.size * 16, transcendentals=0
        ),
        name="finish_part",
    )(own, pairs, scale)


def collect_kernel(x_ref, out_ref, own_sem, send_sem, recv_sem):
    members, peers = send_sem.shape
    depth = x_ref.shape[1]
    place, column = lax.axis_index("ep"), lax.axis_index("tp")
    member = lax.rem(place, members)
    first = place - member

    def peer(step):
        return {"tp": lax.rem(column + step, peers)}

    def partner(step):
        return {"ep": first + lax.rem(member + step, members)}

    def block(owner):
        return out_ref.at[member, :, pl.ds(pl.multiple_of(owner * depth, 128), depth)]

    def send(source, target, m, q, device):
        copy = pltpu.make_async_remote_copy(
            src_ref=source,
            dst_ref=target,
            send_sem=send_sem.at[m, q],
            recv_sem=recv_sem.at[m, q],
            device_id=device,
            device_id_type=pl.DeviceIdType.MESH,
        )
        copy.start()
        return copy

    barrier = pltpu.get_barrier_semaphore()
    others = [peer(q) for q in range(1, peers)] + [partner(m) for m in range(1, members)]
    for device in others:
        pl.semaphore_signal(
            barrier, inc=1, device_id=device, device_id_type=pl.DeviceIdType.MESH
        )
    pl.semaphore_wait(barrier, len(others))
    across = [send(x_ref, block(column), 0, q, peer(q)) for q in range(1, peers)]
    within = [send(x_ref, block(column), m, 0, partner(m)) for m in range(1, members)]
    mine = pltpu.make_async_copy(x_ref, block(column), own_sem)
    mine.start()
    for q in range(1, peers):
        across[q - 1].wait_recv()
        landed = block(lax.rem(column + peers - q, peers))
        for m in range(1, members):
            within.append(send(landed, landed, m, q, partner(m)))
    for copy in across:
        copy.wait_send()
    for copy in within:
        copy.wait()
    mine.wait()


def collect(x, members, collective_id, name):
    rows, depth = x.shape
    peers = lax.axis_size("tp")
    return pl.pallas_call(
        collect_kernel,
        out_shape=jax.ShapeDtypeStruct((members, rows, peers * depth), x.dtype),
        in_specs=[pl.BlockSpec(memory_space=pltpu.VMEM)],
        out_specs=pl.BlockSpec(memory_space=pltpu.VMEM),
        scratch_shapes=[
            pltpu.SemaphoreType.DMA,
            pltpu.SemaphoreType.DMA((members, peers)),
            pltpu.SemaphoreType.DMA((members, peers)),
        ],
        compiler_params=pltpu.CompilerParams(
            collective_id=collective_id, has_side_effects=True
        ),
        cost_estimate=pl.CostEstimate(
            flops=0, bytes_accessed=16 * x.size * members * peers, transcendentals=0
        ),
        name=name,
    )(x).reshape(members * rows, peers * depth)


def blend_sequence(
    reception_vectors,
    lookup_vectors,
    payload_vectors,
    fix_strength_signal,
    fade_signal_term,
    state_erasure,
    feature_speed_pairs,
    subspace_scale_vector,
    subspace_merge_matrix,
):
    def begin(after):
        after, recept = lax.optimization_barrier((after, reception_vectors))
        own, pair = local_part(
            (
                recept,
                lookup_vectors,
                payload_vectors,
                fix_strength_signal,
                fade_signal_term,
                state_erasure,
            ),
            feature_speed_pairs,
        )
        return after, own, lax.all_gather(pair, "ep")

    def finish(own, pairs, after):
        ready, _ = lax.optimization_barrier((own, after))
        mixed_rows = finish_part(ready, pairs, subspace_scale_vector.reshape(1, -1))
        return jnp.dot(
            collect(mixed_rows, 1, 3, "mixed_gather"),
            subspace_merge_matrix,
            preferred_element_type=jnp.float32,
        ).astype(jnp.bfloat16)

    return begin, finish


def expert_layer(
    begin,
    finish,
    specialist_entry_vectors,
    specialist_entry_scale,
    specialist_picks,
    dispatch_replica_share,
    specialist_valve_matrix,
    specialist_raising_matrix,
    specialist_lowering_matrix,
):
    rows_here, model_width = specialist_entry_vectors.shape
    pairs = specialist_picks.shape[1]
    expert_count = lax.axis_size("ep") * specialist_valve_matrix.shape[0]
    per_group = expert_count // GROUPS
    busiest = per_group * max(1, 3 * rows_here // (8 * per_group))
    share = busiest // per_group
    widened = specialist_entry_vectors.astype(jnp.float32)
    inverse = lax.rsqrt(jnp.mean(widened * widened, axis=-1, keepdims=True) + 1e-06)
    depth = model_width // lax.axis_size("tp")
    start = lax.axis_index("tp") * depth
    columns = lax.dynamic_slice_in_dim(specialist_entry_vectors, start, depth, 1)
    gain = lax.dynamic_slice_in_dim(specialist_entry_scale, start, depth, 0)
    normed = (columns.astype(jnp.float32) * inverse * gain).astype(jnp.bfloat16)
    group = specialist_picks[:, 0] // per_group
    earlier = jnp.arange(rows_here)[:, None] > jnp.arange(rows_here)[None, :]
    rank = jnp.sum(((group[:, None] == group[None, :]) & earlier).astype(jnp.int32), axis=1)
    slots = jnp.arange(GROUPS * busiest, dtype=jnp.int32)[:, None]
    placement_mat = (slots == (group * busiest + rank)[None, :]).astype(jnp.bfloat16)
    send_rows = jnp.dot(placement_mat, normed, preferred_element_type=jnp.float32).astype(
        jnp.bfloat16
    )
    send_rows = send_rows.reshape(expert_count, share, depth)
    send_rows, own, pairs = begin(send_rows)
    arrived = lax.all_to_all(send_rows, "ep", split_axis=0, concat_axis=0, tiled=True)
    flat_rows = collect(arrived.reshape(expert_count * share, depth), per_group, 1, "row_gather")
    gate_part = jnp.dot(flat_rows, specialist_valve_matrix[0], preferred_element_type=jnp.float32)
    up_part = jnp.dot(flat_rows, specialist_raising_matrix[0], preferred_element_type=jnp.float32)
    hidden = (jax.nn.silu(gate_part) * up_part).astype(jnp.bfloat16)
    result = jnp.dot(
        collect(hidden, 1, 2, "hidden_gather"),
        specialist_lowering_matrix[0],
        preferred_element_type=jnp.float32,
    ).astype(jnp.bfloat16)
    out_width = result.shape[1]
    result = result.reshape(per_group, expert_count, share, out_width)
    mixed = finish(own, pairs, result)
    returned = lax.all_to_all(
        result.transpose(1, 0, 2, 3).reshape(expert_count, busiest, out_width),
        "ep",
        split_axis=0,
        concat_axis=0,
        tiled=True,
    )
    returned, mixed = lax.optimization_barrier((returned, mixed))
    flat_back = returned.reshape(expert_count * busiest, out_width).astype(jnp.float32)
    expert_of = jnp.arange(expert_count, dtype=jnp.int32)[:, None]
    weight = jnp.sum(
        jnp.where(
            specialist_picks[None] == expert_of[:, :, None], dispatch_replica_share[None], 0.0
        ),
        axis=-1,
    )
    here = jnp.arange(busiest, dtype=jnp.int32)[:, None] == rank[None, :]
    combine_w = jnp.where(here[None], weight[:, None, :], 0.0).reshape(-1, rows_here)
    combined = jnp.einsum("st,sd->td", combine_w, flat_back, precision=highest)
    return mixed, combined.astype(jnp.bfloat16)


def body(
    reception_vectors,
    lookup_vectors,
    payload_vectors,
    fix_strength_signal,
    fade_signal_term,
    state_erasure,
    feature_speed_pairs,
    subspace_scale_vector,
    subspace_merge_matrix,
    specialist_entry_vectors,
    specialist_entry_scale,
    specialist_picks,
    dispatch_replica_share,
    specialist_valve_matrix,
    specialist_raising_matrix,
    specialist_lowering_matrix,
):
    begin, finish = blend_sequence(
        reception_vectors,
        lookup_vectors,
        payload_vectors,
        fix_strength_signal,
        fade_signal_term,
        state_erasure,
        feature_speed_pairs,
        subspace_scale_vector,
        subspace_merge_matrix,
    )
    return expert_layer(
        begin,
        finish,
        specialist_entry_vectors,
        specialist_entry_scale,
        specialist_picks,
        dispatch_replica_share,
        specialist_valve_matrix,
        specialist_raising_matrix,
        specialist_lowering_matrix,
    )


def solution(mesh):
    placed = (
        P("ep", "tp"),
        P("ep", "tp"),
        P("ep", "tp"),
        P("ep", "tp"),
        P("ep", "tp"),
        P("ep", "tp"),
        P(None, "tp"),
        P("tp"),
        P(None, "tp"),
        P("ep", None),
        P(),
        P("ep", None),
        P("ep", None),
        P("ep", None, "tp"),
        P("ep", None, "tp"),
        P("ep", None, "tp"),
    )
    return jax.shard_map(
        body, mesh=mesh, in_specs=placed, out_specs=(P("ep", "tp"), P("ep", "tp")), check_vma=False
    )
```
